32 devices in a mesh: ep: 8 (over z, y), tp: 4 (over x, core).
Axes of the slice: x: 2, y: 2, z: 4, core: 2. Of those that a mesh axis runs over, the one named last changes fastest.
Arguments:
- query_rows: bfloat16 [8192, 1024], P('ep', 'tp'), may hold values from -140 to 140
- key_rows: bfloat16 [8192, 256], P('ep', 'tp'), may hold values from -4.5 to 4.5
- value_rows: bfloat16 [8192, 256], P('ep', 'tp'), may hold values from -6 to 6
- sink_logit: float32 [16], P('tp'), may hold values from 1 to 6
- out_weight: bfloat16 [1024, 2048], P('tp'), may hold values from -0.1875 to 0.1875
- routed_rows: bfloat16 [4096, 2048], P(('ep', 'tp')), may hold values from -6 to 6
- norm_gain: float32 [2048], replicated, may hold values from 0.1 to 1.9
- routing: int32 [4096, 2], P(('ep', 'tp')), may hold values from 0 to 7, all different within a row; in each aligned block of 128 rows (0 to 127, 128 to 255, ...) at most 36 rows name the same one
- route_weight: float32 [4096, 2], P(('ep', 'tp')), may hold values from 0.2 to 1
- gate_weight: bfloat16 [8, 2048, 7168], P('ep', None, 'tp'), may hold values from -0.125 to 0.125
- up_weight: bfloat16 [8, 2048, 7168], P('ep', None, 'tp'), may hold values from -0.125 to 0.125
- down_weight: bfloat16 [8, 7168, 2048], P('ep', 'tp'), may hold values from -0.0625 to 0.0625
Outputs:
- mixed_rows: bfloat16 [8192, 2048], P(('ep', 'tp'))
- expert_mix: bfloat16 [4096, 2048], P(('ep', 'tp'))
The draws below stay inside these ranges and needn't reach their ends.
Inputs may be any that keep to these rules, and one draw needn't show every extreme that they name: `routing`: each token names 2 different experts. Within the 128 rows of one device no expert is named by more than 36 rows, and in every draw some device's rows name some expert exactly 36 times.
All inputs are finite; a program needn't handle non-finite values.
Results may differ from the reference program's by a relative error of at most 0.012.
Values may be sent and summed in bfloat16 or wider, within the bound.
A program may use at most 128 MiB of HBM per device.

```python
import math
import jax
import jax.numpy as jnp
import numpy as np
from jax import lax

D = 2048
HEADS = 16
KV_HEADS = 4
HEAD_DIM = 64
WINDOW = 128
FF = 7168
TOP = 2
MOE_DEV = 128
SEQ = 8192
TOKENS = 4096
EXPERTS = 8
CAP = 36
N_EP = 8
N_TP = 4


def base_pair(key):
    query_base = jnp.clip(jax.random.normal(jax.random.fold_in(key, 11), (SEQ, HEADS * HEAD_DIM), jnp.float32), -4.5, 4.5)
    key_base = jnp.clip(jax.random.normal(jax.random.fold_in(key, 12), (SEQ, KV_HEADS * HEAD_DIM), jnp.float32), -4.5, 4.5)
    return (query_base, key_base)


def draw_query_rows(key, part):
    query_base, key_base = base_pair(key)
    return query_base.astype(jnp.bfloat16)


def draw_key_rows(key, part):
    query_base, key_base = base_pair(key)
    return key_base.astype(jnp.bfloat16)


def levels(own_key, dims, shards, low, largest):
    gain = 1.0
    for position, shards_of in shards:
        heights = jax.random.uniform(jax.random.fold_in(jax.random.fold_in(own_key, 6), position), (shards_of,), jnp.float32, low / len(shards), largest / len(shards))
        gain = gain * jnp.repeat(jnp.exp(heights), dims[position] // shards_of).reshape((-1,) + (1,) * (len(dims) - 1 - position))
    return gain


def shared_out(key, own, number, rows, amount, top, most, slope):
    ranking = jax.random.permutation(key, amount)
    crowded, common = portions_of(amount, rows * top, most, slope, True), portions_of(amount, rows * top, most, slope, False)
    places = jnp.arange(amount)

    def named(lengths, rotation):
        used = int((lengths > 0).sum())
        fixed = max(1, used // 4)
        passed = fixed + (places - fixed + rotation * (used - fixed)) % max(1, amount - fixed)
        return jnp.zeros((amount,), jnp.int32).at[ranking[jnp.where(places < fixed, places, passed)]].set(jnp.asarray(lengths, jnp.int32))

    lengths = jnp.where(number % 4 == 0, named(crowded, number // 4), named(common, number - number // 4 - 1))
    mixed = jax.random.permutation(jax.random.fold_in(own, 3), amount)
    source_of, receiver = mixed[0:amount // 2 * 2:2], mixed[1:amount // 2 * 2:2]
    margin = jnp.minimum(lengths[source_of] - 1, most - lengths[receiver]) // 2
    margin = jnp.where((source_of == ranking[0]) | (receiver == ranking[0]) | (lengths[receiver] == 0), 0, jnp.maximum(margin, 0))
    passed = jax.random.randint(jax.random.fold_in(own, 4), (amount // 2,), 0, 1 << 20) % (margin + 1)
    lengths = lengths.at[source_of].add(-passed).at[receiver].add(passed)
    items = jnp.searchsorted(jnp.cumsum(lengths), jnp.arange(rows * top), side="right").astype(jnp.int32)
    table = items.reshape(top, rows).T
    table = table[jax.random.permutation(jax.random.fold_in(own, 1), rows)]
    rotation = jax.random.randint(jax.random.fold_in(own, 2), (rows, 1), 0, top)
    return jnp.take_along_axis(table, (jnp.arange(top)[None, :] + rotation) % top, axis=1)


def portions_of(number_of, total, most, skew, full):
    weights = [(1 << 20) // math.isqrt(standing ** skew) + 1 for standing in range(1, number_of + 1)]
    largest = most if full else min(most, max(-(-total // number_of), total * weights[0] // sum(weights)))
    least = 1 if total - largest >= number_of - 1 else 0
    counts, rest = [largest] + [least] * (number_of - 1), total - largest - least * (number_of - 1)
    while rest > 0:
        free = [i for i in range(1, number_of) if counts[i] < largest] or [i for i in range(1, number_of) if counts[i] < most]
        pool, left = sum([weights[i] for i in free]), rest
        for i in free:
            addition = min(most - counts[i], max(1, left * weights[i] // pool), rest)
            counts[i] = counts[i] + addition
            rest = rest - addition
    return np.array(counts)


def noise(own_key, extent, spread, bound, split=(), kind=jnp.bfloat16):
    entries = jax.random.normal(own_key, extent, jnp.float32) * spread
    if len(split) > 0:
        entries = levels(own_key, extent, split, -0.22, 0.18) * entries
    return jnp.clip(entries, min=-bound, max=bound).astype(kind)


def setup_inputs(seed: int = 0) -> dict:
    key_list = jax.random.split(jax.random.key(seed), 13)
    query_rows = draw_query_rows(jax.random.fold_in(key_list[12], 71), 0)
    key_rows = draw_key_rows(jax.random.fold_in(key_list[12], 71), 0)
    value_rows = noise(key_list[2], (SEQ, KV_HEADS * HEAD_DIM), 1.0, 6.0, ((0, 8), (1, 4)))
    sink_logit = jnp.clip(1.0 + 5.0 * jax.random.uniform(key_list[3], (HEADS,), jnp.float32) ** levels(key_list[3], (HEADS,), ((0, 4),), -0.2, 0.2), 1.0, 6.0)
    out_weight = noise(key_list[4], (HEADS * HEAD_DIM, D), (HEADS * HEAD_DIM) ** -0.5, 0.1875, ((0, 4),))
    routed_rows = noise(key_list[5], (TOKENS, D), 1.0, 6.0, ((0, 32),))
    norm_gain = jnp.clip(1.0 + 0.18 * jax.random.normal(key_list[6], (D,), jnp.float32), 0.1, 1.9)
    routing_keys = jax.random.split(jax.random.fold_in(key_list[7], 1), TOKENS // MOE_DEV)
    routing_turns = jax.random.permutation(jax.random.fold_in(key_list[7], 3), TOKENS // MOE_DEV)
    routing = jax.vmap(lambda own, number: shared_out(jax.random.fold_in(key_list[7], 2), own, number, MOE_DEV, EXPERTS, TOP, CAP, 0))(routing_keys, routing_turns).reshape((TOKENS, TOP))
    route_weight = jnp.clip(0.2 + 0.8 * jax.random.uniform(key_list[8], (TOKENS, TOP), jnp.float32) ** levels(key_list[8], (TOKENS, TOP), ((0, 32),), -0.2, 0.2), 0.2, 1.0)
    gate_weight = noise(key_list[9], (EXPERTS, D, FF), D ** -0.5, 0.125, ((0, 8), (2, 4)))
    up_weight = noise(key_list[10], (EXPERTS, D, FF), D ** -0.5, 0.125, ((0, 8), (2, 4)))
    down_weight = noise(key_list[11], (EXPERTS, FF, D), FF ** -0.5, 0.0625, ((0, 8), (1, 4)))
    return {"query_rows": query_rows, "key_rows": key_rows, "value_rows": value_rows, "sink_logit": sink_logit, "out_weight": out_weight, "routed_rows": routed_rows, "norm_gain": norm_gain, "routing": routing, "route_weight": route_weight, "gate_weight": gate_weight, "up_weight": up_weight, "down_weight": down_weight}


EPS = 1e-06

def attention_part(query_rows, key_rows, value_rows, sink_logit):
    seq_total = query_rows.shape[0]
    group_size = HEADS // KV_HEADS
    block_rows = min(512, seq_total)
    score_scale = HEAD_DIM ** (-0.5)
    key_pad = jnp.pad(key_rows.astype(jnp.float32), ((WINDOW, WINDOW), (0, 0)))
    value_pad = jnp.pad(value_rows.astype(jnp.float32), ((WINDOW, WINDOW), (0, 0)))
    query_all = query_rows.astype(jnp.float32)
    sink_col = sink_logit.astype(jnp.float32).reshape(KV_HEADS, group_size)[:, :, None]

    def one_block(block_index):
        first_row = block_index * block_rows
        query_block = lax.dynamic_slice_in_dim(query_all, first_row, block_rows, 0).reshape(block_rows, KV_HEADS, group_size, HEAD_DIM)
        key_block = lax.dynamic_slice_in_dim(key_pad, first_row, block_rows + 2 * WINDOW, 0).reshape(-1, KV_HEADS, HEAD_DIM)
        value_block = lax.dynamic_slice_in_dim(value_pad, first_row, block_rows + 2 * WINDOW, 0).reshape(-1, KV_HEADS, HEAD_DIM)
        scores = jnp.einsum('qkgd,skd->kgqs', query_block, key_block) * score_scale
        query_pos = first_row + jnp.arange(block_rows, dtype=jnp.int32)
        key_pos = first_row - WINDOW + jnp.arange(block_rows + 2 * WINDOW, dtype=jnp.int32)
        inside = (jnp.abs(key_pos[None, :] - query_pos[:, None]) <= WINDOW) & (key_pos >= 0)[None, :] & (key_pos < seq_total)[None, :]
        scores = jnp.where(inside, scores, -jnp.inf)
        row_peak = jnp.maximum(lax.optimization_barrier(jnp.max(scores, axis=-1)), sink_col)
        weights = jnp.where(inside, jnp.exp(scores - row_peak[..., None]), 0.0)
        total_weight = lax.optimization_barrier(jnp.sum(weights, axis=-1)) + jnp.exp(sink_col - row_peak)
        rounded = lax.optimization_barrier(weights.astype(jnp.bfloat16)).astype(jnp.float32)
        attended = jnp.einsum('kgqs,skd->qkgd', rounded, value_block) / jnp.transpose(total_weight, (2, 0, 1))[..., None]
        return attended.reshape(block_rows, HEADS * HEAD_DIM).astype(jnp.bfloat16)
    pieces = lax.map(one_block, jnp.arange(seq_total // block_rows, dtype=jnp.int32))
    return pieces.reshape(seq_total, HEADS * HEAD_DIM)

def expert_part(routed_rows, norm_gain, routing, route_weight, gate_weight, up_weight, down_weight):
    token_count = routed_rows.shape[0]
    values = routed_rows.astype(jnp.float32)
    normed = (values * lax.rsqrt(lax.optimization_barrier(jnp.mean(values * values, axis=-1, keepdims=True)) + EPS) * norm_gain.astype(jnp.float32)).astype(jnp.bfloat16)
    slot_limit = N_EP * N_TP * CAP
    shard_width = FF // N_TP

    def per_expert(carry, stacked):
        expert_id, gate_one, up_one, down_one = stacked
        chosen = routing == expert_id
        weight_one = lax.optimization_barrier(jnp.sum(jnp.where(chosen, route_weight.astype(jnp.float32), 0.0), axis=1))
        is_routed = jnp.any(chosen, axis=1)
        slot_place = (jnp.cumsum(is_routed.astype(jnp.int32)) - 1).astype(jnp.int32)
        slot_place = jnp.where(is_routed, slot_place, slot_limit).astype(jnp.int32)
        slot_row = jnp.zeros((slot_limit,), jnp.int32).at[slot_place].set(jnp.arange(token_count, dtype=jnp.int32), mode='drop')
        filled = jnp.arange(slot_limit, dtype=jnp.int32) < jnp.sum(is_routed.astype(jnp.int32))
        gathered = normed[slot_row].astype(jnp.float32)
        gate_pre = jnp.dot(gathered, gate_one.astype(jnp.float32), preferred_element_type=jnp.float32)
        up_pre = jnp.dot(gathered, up_one.astype(jnp.float32), preferred_element_type=jnp.float32)
        hidden = (jax.nn.silu(gate_pre) * up_pre).astype(jnp.bfloat16).astype(jnp.float32)
        summed = jnp.zeros((slot_limit, D), jnp.float32)
        for shard_index in range(N_TP):
            low = shard_index * shard_width
            part_rows = jnp.dot(hidden[:, low:low + shard_width], down_one[low:low + shard_width].astype(jnp.float32), preferred_element_type=jnp.float32)
            summed = summed + lax.optimization_barrier(part_rows.astype(jnp.bfloat16)).astype(jnp.float32)
        scaled = summed * jnp.where(filled, weight_one[slot_row], 0.0)[:, None]
        return (carry.at[slot_row].add(scaled), None)
    mixed_sum, unused = lax.scan(per_expert, jnp.zeros((token_count, D), jnp.float32), (jnp.arange(EXPERTS, dtype=jnp.int32), gate_weight, up_weight, down_weight))
    return mixed_sum.astype(jnp.bfloat16)

def reference(query_rows, key_rows, value_rows, sink_logit, out_weight, routed_rows, norm_gain, routing, route_weight, gate_weight, up_weight, down_weight):
    attended = attention_part(query_rows, key_rows, value_rows, sink_logit)
    mixed_rows = jnp.dot(attended.astype(jnp.float32), out_weight.astype(jnp.float32), preferred_element_type=jnp.float32).astype(jnp.bfloat16)
    expert_mix = expert_part(routed_rows, norm_gain, routing, route_weight, gate_weight, up_weight, down_weight)
    return (mixed_rows, expert_mix)
```

```python
import functools

import jax
import jax.numpy as jnp
from jax import lax
from jax.experimental import pallas as pl
from jax.experimental.pallas import tpu as pltpu
from jax.sharding import PartitionSpec as P

HEAD_DIM = 64
WINDOW = 128
EPS = 1e-06
BF = jnp.bfloat16
F32 = jnp.float32
MESH_ID = pl.DeviceIdType.MESH


def kernel(
    E,
    outgoing,
    q_in,
    kv_in,
    sink,
    wout_in,
    wg_in,
    wu_in,
    wd_in,
    mixed,
    results,
    arr,
    abuf,
    hid,
    wg,
    wu,
    wd,
    part,
    cx,
    cy,
    cz,
    cpre,
    fin,
    qb,
    kvb,
    wout,
    att,
    pp,
    px,
    py,
    pz,
    ppre,
    sem_load,
    a_send,
    a_recv,
    c_send,
    c_recv,
    x_send,
    x_recv,
    xc_send,
    xc_recv,
    h_send,
    h_recv,
    p_send,
    p_recv,
    g_send,
    g_recv,
    z_send,
    z_recv,
    r_send,
    r_recv,
):
    e = lax.axis_index("ep")
    t = lax.axis_index("tp")
    mate = t + 1 - 2 * lax.rem(t, 2)
    cross = lax.rem(t + 2, 4)
    far = lax.rem(mate + 2, 4)
    cap, width = outgoing.shape[1], outgoing.shape[2]
    rows = E * cap
    row_count = kv_in.shape[0]
    kv_width = kv_in.shape[1]
    heads = q_in.shape[0]
    ff = wg_in.shape[2]
    own_rows = row_count // 4

    def remote(src, dst, ssem, rsem, to_e, to_t):
        return pltpu.make_async_remote_copy(
            src_ref=src,
            dst_ref=dst,
            send_sem=ssem,
            recv_sem=rsem,
            device_id=(to_e, to_t),
            device_id_type=MESH_ID,
        )

    loads = [
        pltpu.make_async_copy(kv_in, kvb.at[pl.ds(WINDOW, row_count)], sem_load.at[0]),
        pltpu.make_async_copy(q_in, qb, sem_load.at[1]),
        pltpu.make_async_copy(outgoing.at[e], arr.at[t, e], sem_load.at[2]),
        pltpu.make_async_copy(wout_in, wout, sem_load.at[3]),
        pltpu.make_async_copy(wg_in.at[0], wg, sem_load.at[4]),
        pltpu.make_async_copy(wu_in.at[0], wu, sem_load.at[5]),
        pltpu.make_async_copy(wd_in.at[0], wd, sem_load.at[6]),
    ]
    for copy in loads:
        copy.start()

    barrier = pltpu.get_barrier_semaphore()
    for i in range(1, E):
        pl.semaphore_signal(barrier, inc=1, device_id=(lax.rem(e + i, E), t), device_id_type=MESH_ID)
    pl.semaphore_signal(barrier, inc=1, device_id=(e, mate), device_id_type=MESH_ID)
    pl.semaphore_signal(barrier, inc=1, device_id=(e, cross), device_id_type=MESH_ID)
    pl.semaphore_wait(barrier, E + 1)

    def to_core(i, src):
        s = lax.rem(e + E - i, E)
        return remote(src, arr.at[t, s], c_send.at[i], c_recv.at[i], e, mate)

    def to_cross(i, src):
        s = lax.rem(e + E - i, E)
        return remote(src, arr.at[t, s], x_send.at[i], x_recv.at[i], e, cross)

    def relay(i):
        s = lax.rem(e + E - i, E)
        return remote(arr.at[cross, s], arr.at[cross, s], xc_send.at[i], xc_recv.at[i], e, mate)

    def peer(i):
        d = lax.rem(e + i, E)
        return remote(outgoing.at[d], arr.at[t, e], a_send.at[i], a_recv.at[i], d, t)

    to_cross(0, outgoing.at[e]).start()
    halo_up = remote(
        kv_in.at[pl.ds(row_count - WINDOW, WINDOW)],
        kvb.at[pl.ds(0, WINDOW)],
        h_send.at[0],
        h_recv.at[0],
        lax.rem(e + 1, E),
        t,
    )
    halo_down = remote(
        kv_in.at[pl.ds(0, WINDOW)],
        kvb.at[pl.ds(WINDOW + row_count, WINDOW)],
        h_send.at[1],
        h_recv.at[1],
        lax.rem(e + E - 1, E),
        t,
    )
    halo_up.start()
    halo_down.start()
    for i in range(1, E):
        peer(i).start()
    to_core(0, outgoing.at[e]).start()

    def pump(i):
        peer(i).wait_recv()
        s = lax.rem(e + E - i, E)
        to_cross(i, arr.at[t, s]).start()
        to_core(i, arr.at[t, s]).start()

    def pump_cross(i):
        s = lax.rem(e + E - i, E)
        to_cross(i, arr.at[t, s]).wait_recv()
        relay(i).start()

    loads[0].wait()
    loads[1].wait()
    halo_up.wait_recv()
    halo_down.wait_recv()

    span = 3 * WINDOW
    blocks = row_count // WINDOW
    per_block = E // blocks
    last_block = blocks - 1

    def attention(b):
        start = pl.multiple_of(b * WINDOW, WINDOW)
        keys = kvb[pl.ds(start, span), 0:128]
        vals = kvb[pl.ds(start, span), 128:256]
        lane_v = lax.broadcasted_iota(jnp.int32, (span, 128), 1)
        one = jnp.ones((), BF)
        low_vals = jnp.where(lane_v < HEAD_DIM, vals, one)
        high_vals = jnp.where(lane_v >= HEAD_DIM, vals, one)
        row = lax.broadcasted_iota(jnp.int32, (WINDOW, span), 0)
        col = lax.broadcasted_iota(jnp.int32, (WINDOW, span), 1)
        first = jnp.where((e == 0) & (b == 0), WINDOW, 0)
        last = jnp.where((e == E - 1) & (b == last_block), 2 * WINDOW, span)
        inside = (col >= row) & (col <= row + 2 * WINDOW) & (col >= first) & (col < last)
        lane_o = lax.broadcasted_iota(jnp.int32, (WINDOW, 128), 1)
        outs = []
        for h in range(heads):
            q = qb[h, pl.ds(start, WINDOW), :]
            s = lax.dot_general(q, keys, (((1,), (1,)), ((), ())), preferred_element_type=F32)
            s = jnp.where(inside, s, -jnp.inf)
            sink_h = sink[h]
            peak = jnp.maximum(jnp.max(s, axis=1, keepdims=True), sink_h)
            w = jnp.exp(s - peak).astype(BF)
            rest = jnp.exp(sink_h - peak)
            o = jnp.dot(w, low_vals if h % 2 == 0 else high_vals, preferred_element_type=F32)
            total = (o[:, 127:128] if h % 2 == 0 else o[:, 0:1]) + rest
            outs.append(o / total)
        for pair in range(heads // 2):
            both = jnp.where(lane_o < HEAD_DIM, outs[2 * pair], outs[2 * pair + 1])
            att[pl.ds(start, WINDOW), 128 * pair : 128 * pair + 128] = both.astype(BF)

    def step(b, carry):
        attention(b)
        for k in range(per_block):
            i = b * per_block + k

            @pl.when(i > 0)
            def _():
                pump(i)

        return carry

    lax.fori_loop(0, blocks, step, 0)

    loads[3].wait()

    def project(o):
        a = att[pl.ds(pl.multiple_of(o * own_rows, own_rows), own_rows), :]

        def tile(j, carry):
            c = pl.ds(pl.multiple_of(j * 512, 512), 512)
            pp[o, :, c] = jnp.dot(a, wout[:, c], preferred_element_type=F32).astype(BF)
            return carry

        lax.fori_loop(0, width // 512, tile, 0)

    project(far)
    p_far = remote(pp.at[far], px, p_send.at[0], p_recv.at[0], e, mate)
    p_far.start()
    project(mate)
    p_mate = remote(pp.at[mate], py, p_send.at[1], p_recv.at[1], e, mate)
    p_mate.start()
    project(cross)
    project(t)
    p_far.wait_recv()
    ppre[...] = (pp[cross].astype(F32) + px[...].astype(F32)).astype(BF)

    half = E // 2
    for i in range(half):
        pump_cross(i)
    loads[2].wait()
    loads[4].wait()
    loads[5].wait()

    def expert(o, down_wait=None):
        abuf[...] = arr[o].reshape(rows, width)

        def up_tile(j, carry):
            c = pl.ds(pl.multiple_of(j * 256, 256), 256)
            a = abuf[...]
            g = jnp.dot(a, wg[:, c], preferred_element_type=F32)
            u = jnp.dot(a, wu[:, c], preferred_element_type=F32)
            hid[:, c] = (g / (1.0 + jnp.exp(-g)) * u).astype(BF)
            return carry

        lax.fori_loop(0, ff // 256, up_tile, 0)
        if down_wait is not None:
            down_wait()

        def down_tile(j, carry):
            c = pl.ds(pl.multiple_of(j * 256, 256), 256)
            r = jnp.dot(hid[...], wd[:, c], preferred_element_type=F32)
            for i in range(E):
                part[o, i, :, c] = r[i * cap : (i + 1) * cap].astype(BF)
            return carry

        lax.fori_loop(0, width // 256, down_tile, 0)

    expert(t, loads[6].wait)
    for i in range(half, E - E // 4):
        pump_cross(i)
    for i in range(E):
        to_core(i, arr.at[mate, 0]).wait_recv()
    expert(mate)
    g_mate = remote(part.at[mate], cy, g_send.at[1], g_recv.at[1], e, mate)
    g_mate.start()
    for i in range(E - E // 4, E):
        pump_cross(i)
    p_cross = remote(ppre, pz, p_send.at[2], p_recv.at[2], e, cross)
    p_cross.start()
    for i in range(E):
        relay(i).wait_recv()
    expert(far)
    g_far = remote(part.at[far], cx, g_send.at[0], g_recv.at[0], e, mate)
    g_far.start()
    expert(cross)
    g_far.wait_recv()

    def to_owner(i):
        s = lax.rem(e + i, E)
        return remote(cpre.at[s], cz.at[s], z_send.at[i], z_recv.at[i], e, cross)

    def give_back(i):
        s = lax.rem(e + i, E)
        return remote(fin.at[s], results.at[e], r_send.at[i], r_recv.at[i], s, t)

    order = list(range(1, E)) + [0]
    for i in order:
        s = lax.rem(e + i, E)
        cpre[s] = (part[cross, s].astype(F32) + cx[s].astype(F32)).astype(BF)
        to_owner(i).start()

    g_mate.wait_recv()
    p_mate.wait_recv()
    p_cross.wait_recv()
    mixed[...] = (pp[t].astype(F32) + py[...].astype(F32) + pz[...].astype(F32)).astype(BF)
    for i in order:
        s = lax.rem(e + i, E)
        to_owner(i).wait_recv()
        fin[s] = (part[t, s].astype(F32) + cy[s].astype(F32) + cz[s].astype(F32)).astype(BF)
        if i:
            give_back(i).start()
    keep = pltpu.make_async_copy(fin.at[e], results.at[e], sem_load.at[7])
    keep.start()
    for i in range(1, E):
        give_back(i).wait_recv()
    keep.wait()

    halo_up.wait_send()
    halo_down.wait_send()
    p_far.wait_send()
    p_mate.wait_send()
    p_cross.wait_send()
    g_far.wait_send()
    g_mate.wait_send()
    for i in range(E):
        to_core(i, arr.at[t, 0]).wait_send()
        to_cross(i, arr.at[t, 0]).wait_send()
        relay(i).wait_send()
        to_owner(i).wait_send()
        if i:
            peer(i).wait_send()
            give_back(i).wait_send()


def body(
    query_rows,
    key_rows,
    value_rows,
    sink_logit,
    out_weight,
    routed_rows,
    norm_gain,
    routing,
    route_weight,
    gate_weight,
    up_weight,
    down_weight,
):
    E = lax.axis_size("ep")
    row_count = query_rows.shape[0]
    heads = query_rows.shape[1] // HEAD_DIM
    ff = gate_weight.shape[2]
    q = (query_rows * jnp.asarray(HEAD_DIM**-0.5, BF)).reshape(row_count, heads, HEAD_DIM)
    q = jnp.pad(jnp.transpose(q, (1, 0, 2)), ((0, 0), (0, 0), (0, 128 - HEAD_DIM)))
    kv = jnp.concatenate([key_rows, jnp.zeros_like(key_rows), value_rows, value_rows], axis=1)

    token_count, width = routed_rows.shape
    top = routing.shape[1]
    cap = token_count * top * 9 // (8 * E)
    rows = E * cap
    values = routed_rows.astype(F32)
    normed = (
        values * lax.rsqrt(jnp.mean(values * values, axis=-1, keepdims=True) + EPS) * norm_gain
    ).astype(BF)
    chosen = routing.reshape(-1)
    count = chosen.shape[0]
    earlier = jnp.arange(count)[None, :] < jnp.arange(count)[:, None]
    slot = jnp.sum((earlier & (chosen[None, :] == chosen[:, None])).astype(jnp.int32), axis=1)
    target = (chosen * cap + slot).reshape(token_count, top)
    place = jnp.arange(rows, dtype=jnp.int32)
    hit = target[:, :, None] == place[None, None, :]
    spread = jnp.any(hit, axis=1).astype(BF)
    outgoing = lax.dot_general(
        spread, normed, (((0,), (0,)), ((), ())), preferred_element_type=F32
    ).astype(BF)
    outgoing = outgoing.reshape(E, cap, width)

    own = row_count // 4
    dma = pltpu.SemaphoreType.DMA
    block = (E, cap, width)
    any_spec = pl.BlockSpec(memory_space=pl.ANY)
    mixed, results = pl.pallas_call(
        functools.partial(kernel, E),
        out_shape=(
            jax.ShapeDtypeStruct((own, width), BF),
            jax.ShapeDtypeStruct(block, BF),
        ),
        in_specs=[
            any_spec,
            any_spec,
            any_spec,
            pl.BlockSpec(memory_space=pltpu.SMEM),
            any_spec,
            any_spec,
            any_spec,
            any_spec,
        ],
        out_specs=(pl.BlockSpec(memory_space=pltpu.VMEM), any_spec),
        scratch_shapes=[
            pltpu.VMEM((4,) + block, BF),
            pltpu.VMEM((rows, width), BF),
            pltpu.VMEM((rows, ff), BF),
            pltpu.VMEM((width, ff), BF),
            pltpu.VMEM((width, ff), BF),
            pltpu.VMEM((ff, width), BF),
            pltpu.VMEM((4,) + block, BF),
            pltpu.VMEM(block, BF),
            pltpu.VMEM(block, BF),
            pltpu.VMEM(block, BF),
            pltpu.VMEM(block, BF),
            pltpu.VMEM(block, BF),
            pltpu.VMEM(q.shape, BF),
            pltpu.VMEM((row_count + 2 * WINDOW, kv.shape[1]), BF),
            pltpu.VMEM(out_weight.shape, BF),
            pltpu.VMEM(query_rows.shape, BF),
            pltpu.VMEM((4, own, width), BF),
            pltpu.VMEM((own, width), BF),
            pltpu.VMEM((own, width), BF),
            pltpu.VMEM((own, width), BF),
            pltpu.VMEM((own, width), BF),
            dma((8,)),
            dma((E,)),
            dma((E,)),
            dma((E,)),
            dma((E,)),
            dma((E,)),
            dma((E,)),
            dma((E,)),
            dma((E,)),
            dma((2,)),
            dma((2,)),
            dma((3,)),
            dma((3,)),
            dma((2,)),
            dma((2,)),
            dma((E,)),
            dma((E,)),
            dma((E,)),
            dma((E,)),
        ],
        compiler_params=pltpu.CompilerParams(
            collective_id=0, has_side_effects=True, vmem_limit_bytes=64 * 1024 * 1024 - 131072
        ),
    )(outgoing, q, kv, sink_logit, out_weight, gate_weight, up_weight, down_weight)

    weight = jnp.sum(jnp.where(hit, route_weight[:, :, None], 0.0), axis=1)
    expert_mix = jnp.dot(
        weight,
        results.reshape(rows, width).astype(F32),
        precision=lax.Precision.HIGHEST,
        preferred_element_type=F32,
    ).astype(BF)
    return (mixed, expert_mix)


def solution(mesh):
    in_specs = (
        P("ep", "tp"),
        P("ep", "tp"),
        P("ep", "tp"),
        P("tp"),
        P("tp", None),
        P(("ep", "tp"), None),
        P(),
        P(("ep", "tp"), None),
        P(("ep", "tp"), None),
        P("ep", None, "tp"),
        P("ep", None, "tp"),
        P("ep", "tp", None),
    )
    out_specs = (P(("ep", "tp"), None), P(("ep", "tp"), None))
    return jax.shard_map(body, mesh=mesh, in_specs=in_specs, out_specs=out_specs, check_vma=False)
```
